32 devices in a mesh: sp: 8 (over z, x), tp: 4 (over y, core).
Axes of the slice: x: 2, y: 2, z: 4, core: 2. Of those that a mesh axis runs over, the one named last changes fastest.
Arguments:
- layer_input: bfloat16 [4, 2048, 2048], P(None, ('sp', 'tp')), as said below
- key_weight: bfloat16 [2048, 384], replicated, may hold values from -0.125 to 0.125
- value_weight: bfloat16 [2048, 384], replicated, may hold values from -0.125 to 0.125
- queries: bfloat16 [24, 5, 64], P('sp'), may hold values from -6 to 6
- head_bias: float32 [6, 5], replicated, as said below
Outputs:
- stored: bfloat16 [24, 8, 256, 128], P('sp', None, 'tp')
- first_read: bfloat16 [24, 320], P('sp')
The draws below stay inside these ranges and needn't reach their ends.
Inputs may be any that keep to these rules, and one draw needn't show every extreme that they name: `layer_input`: entries lie between -12.5 and 12.5. `head_bias`: entries lie between -1 minus the natural logarithm of 2048 and -3.
All inputs are finite; a program needn't handle non-finite values.
Results may differ from the reference program's by a relative error of at most 0.01.
Values may be sent and summed in bfloat16 or wider, within the bound.
A program may use at most 64 MiB of HBM per device.

```python
import math
import jax
import jax.numpy as jnp
from jax import lax

D = 2048
HD = 64
KVH = 6
GROUP = 5
SUB = 64
SEQS = 4
PAIRS = 24
LEN = 2048
BLOCKS = 8
SPAN = 256


def draw_layer_input(key, part):
    base_key, scale_key = jax.random.split(key)
    blocks = LEN // SUB
    log_scale = jax.random.uniform(scale_key, (SEQS, blocks, 1, 1), jnp.float32, -0.7, 0.7)
    base = jnp.clip(jax.random.normal(base_key, (SEQS, blocks, SUB, D), jnp.float32), -6.0, 6.0)
    return (base * jnp.exp(log_scale)).reshape(SEQS, LEN, D).astype(jnp.bfloat16)


def draw_head_bias(key, part):
    kind_key, fast_key, slow_key = jax.random.split(key, 3)
    quick = jax.random.randint(kind_key, (KVH, GROUP), 0, 2) == 1
    fast = -math.log(40.0) + jax.random.uniform(fast_key, (KVH, GROUP), jnp.float32, -0.5, 0.5)
    slow = -math.log(LEN) - 0.5 + jax.random.uniform(slow_key, (KVH, GROUP), jnp.float32, -0.5, 0.5)
    return jnp.where(quick, fast, slow).astype(jnp.float32)


def shard_levels(rng, dims, cuts, least, top_value):
    def one(axis_at, parts):
        steps = jax.random.uniform(jax.random.fold_in(jax.random.fold_in(rng, 6), axis_at), (parts,), jnp.float32, least / len(cuts), top_value / len(cuts))
        return jnp.repeat(jnp.exp(steps), dims[axis_at] // parts).reshape((-1,) + (1,) * (len(dims) - axis_at - 1))

    level = one(*cuts[0])
    for cut in cuts[1:]:
        level = level * one(*cut)
    return level


def noise(own_key, dims, scale, most, cuts=(), held_as=jnp.bfloat16):
    factor_of = shard_levels(own_key, dims, cuts, -0.22, 0.18) if cuts else 1.0
    array = jax.random.normal(own_key, dims, jnp.float32) * scale * factor_of
    return jnp.minimum(jnp.maximum(array, -most), most).astype(held_as)


def setup_inputs(seed: int = 0) -> dict:
    streams_of = jax.random.split(jax.random.key(seed), 6)
    return {
        "layer_input": draw_layer_input(jax.random.fold_in(streams_of[5], 71), 0),
        "key_weight": noise(streams_of[1], (D, KVH * HD), D ** -0.5, 0.125),
        "value_weight": noise(streams_of[2], (D, KVH * HD), D ** -0.5, 0.125),
        "queries": noise(streams_of[3], (PAIRS, GROUP, HD), 1.0, 6.0, ((0, 8),)),
        "head_bias": draw_head_bias(jax.random.fold_in(streams_of[5], 71), 0),
    }


EPS_NORM = 0.0001

def reference(layer_input, key_weight, value_weight, queries, head_bias):
    tokens_flat = layer_input.reshape(SEQS * LEN, D)
    key_rows = jnp.dot(tokens_flat, key_weight, preferred_element_type=jnp.float32).astype(jnp.bfloat16).reshape(SEQS, LEN, KVH, HD)
    value_rows = jnp.dot(tokens_flat, value_weight, preferred_element_type=jnp.float32).astype(jnp.bfloat16).reshape(SEQS, LEN, KVH, HD)
    kv_rows = jnp.concatenate([key_rows, value_rows], axis=-1).transpose(0, 2, 1, 3).reshape(PAIRS, LEN, 2 * HD)
    head_shift = jnp.tile(head_bias, (SEQS, 1))
    score_scale = 1.0 / math.sqrt(HD)

    def read_pair(item):
        query, pair_rows, shift = item
        scores = jnp.dot(query, pair_rows[:, :HD].T, preferred_element_type=jnp.float32) * score_scale + shift[:, None]
        keep_log = jax.nn.log_sigmoid(-scores)
        suffix_log = lax.cumsum(keep_log, axis=1, reverse=True) - keep_log
        weights = jnp.exp(jax.nn.log_sigmoid(scores) + suffix_log).astype(jnp.bfloat16)
        return jnp.dot(weights, pair_rows[:, HD:], preferred_element_type=jnp.float32)
    summed = lax.map(read_pair, (queries, kv_rows, head_shift))
    squares = lax.optimization_barrier(jnp.mean(summed * summed, axis=-1, keepdims=True))
    first_read = (summed * lax.rsqrt(squares + EPS_NORM)).reshape(PAIRS, GROUP * HD).astype(jnp.bfloat16)
    return (kv_rows.reshape(PAIRS, BLOCKS, SPAN, 2 * HD), first_read)
```

```python
import functools
import math

import jax
import jax.numpy as jnp
from jax import lax
from jax.experimental import pallas as pl
from jax.experimental.pallas import tpu as pltpu
from jax.sharding import PartitionSpec as P

EPS_NORM = 0.0001
MESH = pl.DeviceIdType.MESH
KC = 4
ROWS = 8


def flip(index, k):
    bit = 1
    while bit <= k:
        if k & bit:
            index = index + (1 - 2 * ((index // bit) % 2)) * bit
        bit *= 2
    return index


def kernel(
    sp, tp, seqs, sub, hd, kvh, group, pairs,
    x_hbm, wk_hbm, wv_hbm, q_hbm, bias_hbm,
    stored_hbm, first_ref,
    x_v, wk_v, wv_v, q_v, bias_v, send, recv, msg, fin,
    x_sem, w_sem, small_sem, send_sem, recv_sem, msend_sem, mrecv_sem, out_sem,
):
    me = lax.axis_index("sp")
    mt = lax.axis_index("tp")
    per_seq = kvh // pairs
    width = x_hbm.shape[1]
    kc = width // KC
    half_rows = seqs * sub // 2

    barrier = pltpu.get_barrier_semaphore()
    for k in range(1, sp):
        pl.semaphore_signal(barrier, inc=1, device_id={"sp": flip(me, k)}, device_id_type=MESH)
    for k in range(1, tp):
        pl.semaphore_signal(barrier, inc=1, device_id={"tp": lax.rem(mt + k, tp)}, device_id_type=MESH)

    top = me // (sp // 2)
    far_row = pl.multiple_of((1 - top) * half_rows, half_rows)
    near_row = pl.multiple_of(top * half_rows, half_rows)

    x_far = pltpu.make_async_copy(x_hbm.at[pl.ds(far_row, half_rows)], x_v.at[pl.ds(far_row, half_rows)], x_sem.at[0])
    x_near = pltpu.make_async_copy(x_hbm.at[pl.ds(near_row, half_rows)], x_v.at[pl.ds(near_row, half_rows)], x_sem.at[1])
    x_far.start()
    w_copies = []
    for c in range(KC):
        rows = pl.ds(c * kc, kc)
        a = pltpu.make_async_copy(wk_hbm.at[rows], wk_v.at[rows], w_sem.at[0, c])
        b = pltpu.make_async_copy(wv_hbm.at[rows], wv_v.at[rows], w_sem.at[1, c])
        a.start()
        b.start()
        w_copies.append((a, b))
    x_near.start()
    q_copy = pltpu.make_async_copy(q_hbm, q_v, small_sem.at[0])
    bias_copy = pltpu.make_async_copy(bias_hbm, bias_v, small_sem.at[1])
    q_copy.start()
    bias_copy.start()

    def project(row0):
        return project_cols(row0)

    def pieces(keys, values, i, part):
        out = []
        for p in range(pairs):
            c0 = (part * pairs + p) * hd
            out.append(keys[i * sub:(i + 1) * sub, c0:c0 + hd])
            out.append(values[i * sub:(i + 1) * sub, c0:c0 + hd])
        return jnp.concatenate(out, axis=1).astype(jnp.bfloat16)

    x_far.wait()
    keys = values = None
    for c in range(KC):
        w_copies[c][0].wait()
        w_copies[c][1].wait()
        xc = x_v[pl.ds(far_row, half_rows), c * kc:(c + 1) * kc]
        dk = jnp.dot(xc, wk_v[c * kc:(c + 1) * kc, :], preferred_element_type=jnp.float32)
        dv = jnp.dot(xc, wv_v[c * kc:(c + 1) * kc, :], preferred_element_type=jnp.float32)
        keys = dk if keys is None else keys + dk
        values = dv if values is None else values + dv
    far_base = (1 - top) * (sp // 2)
    for i in range(seqs // 2):
        for part in range(per_seq):
            send[pl.ds(far_base + i * per_seq + part, 1)] = pieces(keys, values, i, part)[None]

    pl.semaphore_wait(barrier, sp + tp - 2)

    def block_copy(k):
        to = flip(me, k)
        return pltpu.make_async_remote_copy(
            src_ref=send.at[to], dst_ref=recv.at[me],
            send_sem=send_sem.at[to], recv_sem=recv_sem.at[me],
            device_id={"sp": to}, device_id_type=MESH,
        )

    def arrived(k):
        frm = flip(me, k)
        return pltpu.make_async_remote_copy(
            src_ref=send.at[frm], dst_ref=recv.at[frm],
            send_sem=send_sem.at[frm], recv_sem=recv_sem.at[frm],
            device_id={"sp": frm}, device_id_type=MESH,
        )

    for k in range(sp // 2, sp):
        block_copy(k).start()

    x_near.wait()
    xn = x_v[pl.ds(near_row, half_rows), :]
    keys = jnp.dot(xn, wk_v[...], preferred_element_type=jnp.float32)
    values = jnp.dot(xn, wv_v[...], preferred_element_type=jnp.float32)
    near_base = top * (sp // 2)
    for i in range(seqs // 2):
        for part in range(per_seq):
            send[pl.ds(near_base + i * per_seq + part, 1)] = pieces(keys, values, i, part)[None]
    for k in range(1, sp // 2):
        block_copy(k).start()
    recv[pl.ds(me, 1)] = send[pl.ds(me, 1)]

    q_copy.wait()
    bias_copy.wait()
    h0 = lax.rem(me * pairs, kvh)
    eye = lax.broadcasted_iota(jnp.int32, (ROWS, group), 0) == lax.broadcasted_iota(jnp.int32, (ROWS, group), 1)
    q_pads = []
    shifts = []
    for p in range(pairs):
        qp = q_v[p].astype(jnp.float32)
        qp = jnp.concatenate([qp, jnp.zeros((group, hd), jnp.float32)], axis=1)
        qp = jnp.concatenate([qp, jnp.zeros((ROWS - group, 2 * hd), jnp.float32)], axis=0)
        q_pads.append(qp.astype(jnp.bfloat16))
        row = bias_v[pl.ds(h0 + p, 1), :]
        shifts.append(jnp.sum(jnp.where(eye, jnp.broadcast_to(row, (ROWS, group)), 0.0), axis=1, keepdims=True))
    shift = jnp.concatenate(shifts, axis=0)
    scale = 1.0 / math.sqrt(hd)
    later = lax.broadcasted_iota(jnp.int32, (sub, 256), 0)
    column = lax.broadcasted_iota(jnp.int32, (sub, 256), 1)
    tri = ((later > column) | (column >= 128)).astype(jnp.float32).astype(jnp.bfloat16)
    left_half = lax.broadcasted_iota(jnp.int32, (pairs * ROWS, 2 * hd), 1) < hd

    def msg_copy(b, t):
        return pltpu.make_async_remote_copy(
            src_ref=msg.at[mt, b], dst_ref=msg.at[mt, b],
            send_sem=msend_sem.at[t, b], recv_sem=mrecv_sem.at[mt, b],
            device_id={"tp": t}, device_id_type=MESH,
        )

    def msg_arrived(b, t):
        return pltpu.make_async_remote_copy(
            src_ref=msg.at[t, b], dst_ref=msg.at[t, b],
            send_sem=msend_sem.at[t, b], recv_sem=mrecv_sem.at[t, b],
            device_id={"tp": t}, device_id_type=MESH,
        )

    def out_copies(b):
        return [
            pltpu.make_async_copy(recv.at[b, :, pl.ds(p * 2 * hd, 2 * hd)], stored_hbm.at[p, b], out_sem.at[b, p])
            for p in range(pairs)
        ]

    def attend(b):
        scores = []
        for p in range(pairs):
            kv = recv[b, :, p * 2 * hd:(p + 1) * 2 * hd]
            scores.append(lax.dot_general(q_pads[p], kv, (((1,), (1,)), ((), ())), preferred_element_type=jnp.float32))
        s = jnp.concatenate(scores, axis=0) * scale + shift
        low = jnp.log1p(jnp.exp(-jnp.abs(s)))
        keep = -(jnp.maximum(s, 0.0) + low)
        sig = jnp.minimum(s, 0.0) - low
        hi = keep.astype(jnp.bfloat16)
        rest = keep - hi.astype(jnp.float32)
        mid = rest.astype(jnp.bfloat16)
        lo = (rest - mid.astype(jnp.float32)).astype(jnp.bfloat16)
        n = pairs * ROWS
        sums = (
            jnp.dot(hi, tri, preferred_element_type=jnp.float32)
            + jnp.dot(mid, tri, preferred_element_type=jnp.float32)
            + jnp.dot(lo, tri, preferred_element_type=jnp.float32)
        )
        weights = jnp.exp(sig + sums[:, :sub]).astype(jnp.bfloat16)
        reads = []
        for p in range(pairs):
            kv = recv[b, :, p * 2 * hd:(p + 1) * 2 * hd]
            reads.append(jnp.dot(weights[p * ROWS:(p + 1) * ROWS], kv, preferred_element_type=jnp.float32))
        read = jnp.concatenate(reads, axis=0)
        msg[mt, b] = jnp.where(left_half, sums[:, 128:128 + 2 * hd], read)
        for t in range(1, tp):
            msg_copy(b, lax.rem(mt + t, tp)).start()

    order = [0] + list(range(1, sp))
    for k in order:
        b = flip(me, k)
        if k:
            arrived(k).wait_recv()
        for copy in out_copies(b):
            copy.start()
        attend(b)

    for b in range(sp):
        for t in range(1, tp):
            msg_arrived(b, lax.rem(mt + t, tp)).wait_recv()

    def add_block(i, carry):
        total, acc = carry
        b = sp - 1 - i
        for j in range(tp - 1, -1, -1):
            m = msg[j, b]
            total = total + jnp.exp(acc) * m
            acc = acc + pltpu.roll(m, hd, 1)
        return total, acc

    zero = jnp.zeros((pairs * ROWS, 2 * hd), jnp.float32)
    total, _ = lax.fori_loop(0, sp, add_block, (zero, zero), unroll=True)
    total = jnp.where(left_half, 0.0, total)
    squares = jnp.sum(total * total, axis=1, keepdims=True) * (1.0 / hd)
    fin[...] = pltpu.roll(total * lax.rsqrt(squares + EPS_NORM), hd, 1)
    cols = [fin[pl.ds(g, pairs, stride=ROWS), :][:, :hd] for g in range(group)]
    first_ref[...] = jnp.concatenate(cols, axis=1).astype(first_ref.dtype)

    for k in range(1, sp):
        block_copy(k).wait_send()
    for b in range(sp):
        for t in range(1, tp):
            msg_copy(b, lax.rem(mt + t, tp)).wait_send()
        for copy in out_copies(b):
            copy.wait()


def solution(mesh):
    sp, tp = mesh.shape["sp"], mesh.shape["tp"]

    def per_device(layer_input, key_weight, value_weight, queries, head_bias):
        seqs, sub, width = layer_input.shape
        pairs, group, hd = queries.shape
        kvh = head_bias.shape[0]
        x = layer_input.reshape(seqs * sub, width)
        block = pairs * 2 * hd
        any_spec = pl.BlockSpec(memory_space=pl.ANY)
        dma = pltpu.SemaphoreType.DMA
        stored, first = pl.pallas_call(
            functools.partial(kernel, sp, tp, seqs, sub, hd, kvh, group, pairs),
            out_shape=(
                jax.ShapeDtypeStruct((pairs, sp, sub, 2 * hd), jnp.bfloat16),
                jax.ShapeDtypeStruct((pairs, group * hd), jnp.bfloat16),
            ),
            in_specs=[any_spec] * 5,
            out_specs=(any_spec, pl.BlockSpec(memory_space=pltpu.VMEM)),
            scratch_shapes=[
                pltpu.VMEM(x.shape, jnp.bfloat16),
                pltpu.VMEM(key_weight.shape, jnp.bfloat16),
                pltpu.VMEM(value_weight.shape, jnp.bfloat16),
                pltpu.VMEM(queries.shape, jnp.bfloat16),
                pltpu.VMEM(head_bias.shape, jnp.float32),
                pltpu.VMEM((sp, sub, block), jnp.bfloat16),
                pltpu.VMEM((sp, sub, block), jnp.bfloat16),
                pltpu.VMEM((tp, sp, pairs * ROWS, 2 * hd), jnp.float32),
                pltpu.VMEM((pairs * ROWS, 2 * hd), jnp.float32),
                dma((2,)),
                dma((2, KC)),
                dma((2,)),
                dma((sp,)),
                dma((sp,)),
                dma((tp, sp)),
                dma((tp, sp)),
                dma((sp, pairs)),
            ],
            compiler_params=pltpu.CompilerParams(collective_id=0, has_side_effects=True),
        )(x, key_weight, value_weight, queries, head_bias)
        return stored, first

    in_specs = (P(None, ("sp", "tp"), None), P(), P(), P("sp", None, None), P())
    out_specs = (P("sp", None, "tp", None), P("sp", None))
    return jax.shard_map(per_device, mesh=mesh, in_specs=in_specs, out_specs=out_specs, check_vma=False)
```

```python
import functools
import math

import jax
import jax.numpy as jnp
from jax import lax
from jax.experimental import pallas as pl
from jax.experimental.pallas import tpu as pltpu
from jax.sharding import PartitionSpec as P

EPS_NORM = 0.0001
MESH = pl.DeviceIdType.MESH
KC = 4
VMEM_BYTES = 60 * 1024 * 1024
ROWS = 8


def flip(index, k):
    bit = 1
    while bit <= k:
        if k & bit:
            index = index + (1 - 2 * ((index // bit) % 2)) * bit
        bit *= 2
    return index


def kernel(
    sp, tp, seqs, sub, hd, kvh, group, pairs,
    x_hbm, wk_hbm, wv_hbm, q_hbm, bias_hbm,
    recv, msg,
    x_v, wk_v, wv_v, q_v, bias_v, send,
    x_sem, w_sem, small_sem, send_sem, recv_sem, msend_sem, mrecv_sem,
):
    me = lax.axis_index("sp")
    mt = lax.axis_index("tp")
    per_seq = kvh // pairs
    width = x_hbm.shape[1]
    kc = width // KC
    half_rows = seqs * sub // 2

    barrier = pltpu.get_barrier_semaphore()
    for k in range(1, sp):
        pl.semaphore_signal(barrier, inc=1, device_id={"sp": flip(me, k)}, device_id_type=MESH)
    for k in range(1, tp):
        pl.semaphore_signal(barrier, inc=1, device_id={"tp": lax.rem(mt + k, tp)}, device_id_type=MESH)

    top = me // (sp // 2)
    far_row = pl.multiple_of((1 - top) * half_rows, half_rows)
    near_row = pl.multiple_of(top * half_rows, half_rows)

    x_far = pltpu.make_async_copy(x_hbm.at[pl.ds(far_row, half_rows)], x_v.at[pl.ds(far_row, half_rows)], x_sem.at[0])
    x_near = pltpu.make_async_copy(x_hbm.at[pl.ds(near_row, half_rows)], x_v.at[pl.ds(near_row, half_rows)], x_sem.at[1])
    x_far.start()
    w_copies = []
    for c in range(KC):
        rows = pl.ds(c * kc, kc)
        a = pltpu.make_async_copy(wk_hbm.at[rows], wk_v.at[rows], w_sem.at[0, c])
        b = pltpu.make_async_copy(wv_hbm.at[rows], wv_v.at[rows], w_sem.at[1, c])
        a.start()
        b.start()
        w_copies.append((a, b))
    x_near.start()
    q_copy = pltpu.make_async_copy(q_hbm, q_v, small_sem.at[0])
    bias_copy = pltpu.make_async_copy(bias_hbm, bias_v, small_sem.at[1])
    q_copy.start()
    bias_copy.start()

    def pieces(keys, values, i, part):
        out = []
        for p in range(pairs):
            c0 = (part * pairs + p) * hd
            out.append(keys[i * sub:(i + 1) * sub, c0:c0 + hd])
            out.append(values[i * sub:(i + 1) * sub, c0:c0 + hd])
        return jnp.concatenate(out, axis=1).astype(jnp.bfloat16)

    x_far.wait()
    keys = values = None
    for c in range(KC):
        w_copies[c][0].wait()
        w_copies[c][1].wait()
        xc = x_v[pl.ds(far_row, half_rows), c * kc:(c + 1) * kc]
        dk = jnp.dot(xc, wk_v[c * kc:(c + 1) * kc, :], preferred_element_type=jnp.float32)
        dv = jnp.dot(xc, wv_v[c * kc:(c + 1) * kc, :], preferred_element_type=jnp.float32)
        keys = dk if keys is None else keys + dk
        values = dv if values is None else values + dv
    far_base = (1 - top) * (sp // 2)
    for i in range(seqs // 2):
        for part in range(per_seq):
            send[pl.ds(far_base + i * per_seq + part, 1)] = pieces(keys, values, i, part)[None]

    pl.semaphore_wait(barrier, sp + tp - 2)

    def block_copy(k):
        to = flip(me, k)
        return pltpu.make_async_remote_copy(
            src_ref=send.at[to], dst_ref=recv.at[me],
            send_sem=send_sem.at[to], recv_sem=recv_sem.at[me],
            device_id={"sp": to}, device_id_type=MESH,
        )

    def arrived(k):
        frm = flip(me, k)
        return pltpu.make_async_remote_copy(
            src_ref=send.at[frm], dst_ref=recv.at[frm],
            send_sem=send_sem.at[frm], recv_sem=recv_sem.at[frm],
            device_id={"sp": frm}, device_id_type=MESH,
        )

    for k in range(sp // 2, sp):
        block_copy(k).start()

    x_near.wait()
    xn = x_v[pl.ds(near_row, half_rows), :]
    keys = jnp.dot(xn, wk_v[...], preferred_element_type=jnp.float32)
    values = jnp.dot(xn, wv_v[...], preferred_element_type=jnp.float32)
    near_base = top * (sp // 2)
    for i in range(seqs // 2):
        for part in range(per_seq):
            send[pl.ds(near_base + i * per_seq + part, 1)] = pieces(keys, values, i, part)[None]
    for k in range(1, sp // 2):
        block_copy(k).start()
    recv[pl.ds(me, 1)] = send[pl.ds(me, 1)]

    q_copy.wait()
    bias_copy.wait()
    h0 = lax.rem(me * pairs, kvh)
    eye = lax.broadcasted_iota(jnp.int32, (ROWS, group), 0) == lax.broadcasted_iota(jnp.int32, (ROWS, group), 1)
    q_pads = []
    shifts = []
    for p in range(pairs):
        qp = q_v[:, p, :].astype(jnp.float32)
        qp = jnp.concatenate([qp, jnp.zeros((group, hd), jnp.float32)], axis=1)
        qp = jnp.concatenate([qp, jnp.zeros((ROWS - group, 2 * hd), jnp.float32)], axis=0)
        q_pads.append(qp.astype(jnp.bfloat16))
        row = bias_v[pl.ds(h0 + p, 1), :]
        shifts.append(jnp.sum(jnp.where(eye, jnp.broadcast_to(row, (ROWS, group)), 0.0), axis=1, keepdims=True))
    shift = jnp.concatenate(shifts, axis=0)
    scale = 1.0 / math.sqrt(hd)
    later = lax.broadcasted_iota(jnp.int32, (sub, 256), 0)
    column = lax.broadcasted_iota(jnp.int32, (sub, 256), 1)
    tri = ((later > column) | (column >= 128)).astype(jnp.float32).astype(jnp.bfloat16)
    left_half = lax.broadcasted_iota(jnp.int32, (pairs * ROWS, 2 * hd), 1) < hd

    def msg_copy(b, t):
        return pltpu.make_async_remote_copy(
            src_ref=msg.at[mt, b], dst_ref=msg.at[mt, b],
            send_sem=msend_sem.at[t, b], recv_sem=mrecv_sem.at[mt, b],
            device_id={"tp": t}, device_id_type=MESH,
        )

    def msg_arrived(b, t):
        return pltpu.make_async_remote_copy(
            src_ref=msg.at[t, b], dst_ref=msg.at[t, b],
            send_sem=msend_sem.at[t, b], recv_sem=mrecv_sem.at[t, b],
            device_id={"tp": t}, device_id_type=MESH,
        )

    def attend(b):
        scores = []
        for p in range(pairs):
            kv = recv[b, :, p * 2 * hd:(p + 1) * 2 * hd]
            scores.append(lax.dot_general(q_pads[p], kv, (((1,), (1,)), ((), ())), preferred_element_type=jnp.float32))
        s = jnp.concatenate(scores, axis=0) * scale + shift
        low = jnp.log1p(jnp.exp(-jnp.abs(s)))
        keep = -(jnp.maximum(s, 0.0) + low)
        sig = jnp.minimum(s, 0.0) - low
        hi = keep.astype(jnp.bfloat16)
        rest = keep - hi.astype(jnp.float32)
        mid = rest.astype(jnp.bfloat16)
        lo = (rest - mid.astype(jnp.float32)).astype(jnp.bfloat16)
        n = pairs * ROWS
        sums = (
            jnp.dot(hi, tri, preferred_element_type=jnp.float32)
            + jnp.dot(mid, tri, preferred_element_type=jnp.float32)
            + jnp.dot(lo, tri, preferred_element_type=jnp.float32)
        )
        weights = jnp.exp(sig + sums[:, :sub]).astype(jnp.bfloat16)
        reads = []
        for p in range(pairs):
            kv = recv[b, :, p * 2 * hd:(p + 1) * 2 * hd]
            reads.append(jnp.dot(weights[p * ROWS:(p + 1) * ROWS], kv, preferred_element_type=jnp.float32))
        read = jnp.concatenate(reads, axis=0)
        msg[mt, b] = jnp.where(left_half, sums[:, 128:128 + 2 * hd], read)
        for t in range(1, tp):
            msg_copy(b, lax.rem(mt + t, tp)).start()

    order = [0] + list(range(1, sp))
    for k in order:
        b = flip(me, k)
        if k:
            arrived(k).wait_recv()
        attend(b)

    for b in range(sp):
        for t in range(1, tp):
            msg_arrived(b, lax.rem(mt + t, tp)).wait_recv()

    for k in range(1, sp):
        block_copy(k).wait_send()
    for b in range(sp):
        for t in range(1, tp):
            msg_copy(b, lax.rem(mt + t, tp)).wait_send()


def finish(sp, tp, hd, group, pairs, recv, msg, stored_hbm, first_ref, fin, out_sem):
    copies = [
        pltpu.make_async_copy(recv.at[b, :, pl.ds(p * 2 * hd, 2 * hd)], stored_hbm.at[p, b], out_sem.at[b, p])
        for b in range(sp)
        for p in range(pairs)
    ]
    for copy in copies:
        copy.start()
    left_half = lax.broadcasted_iota(jnp.int32, (pairs * ROWS, 2 * hd), 1) < hd

    def add_block(i, carry):
        total, acc = carry
        b = sp - 1 - i
        for j in range(tp - 1, -1, -1):
            m = msg[j, b]
            total = total + jnp.exp(acc) * m
            acc = acc + pltpu.roll(m, hd, 1)
        return total, acc

    zero = jnp.zeros((pairs * ROWS, 2 * hd), jnp.float32)
    total, _ = lax.fori_loop(0, sp, add_block, (zero, zero), unroll=True)
    total = jnp.where(left_half, 0.0, total)
    squares = jnp.sum(total * total, axis=1, keepdims=True) * (1.0 / hd)
    fin[...] = pltpu.roll(total * lax.rsqrt(squares + EPS_NORM), hd, 1)
    cols = [fin[pl.ds(g, pairs, stride=ROWS), :][:, :hd] for g in range(group)]
    first_ref[...] = jnp.concatenate(cols, axis=1).astype(first_ref.dtype)

    for copy in copies:
        copy.wait()


def solution(mesh):
    sp, tp = mesh.shape["sp"], mesh.shape["tp"]

    def per_device(layer_input, key_weight, value_weight, queries, head_bias):
        seqs, sub, width = layer_input.shape
        pairs, group, hd = queries.shape
        kvh = head_bias.shape[0]
        x = layer_input.reshape(seqs * sub, width)
        block = pairs * 2 * hd
        any_spec = pl.BlockSpec(memory_space=pltpu.HBM)
        dma = pltpu.SemaphoreType.DMA
        handed = sp * sub * block * 2 + tp * sp * pairs * ROWS * 2 * hd * 4
        limit = VMEM_BYTES - handed
        vmem_spec = pl.BlockSpec(memory_space=pltpu.VMEM)
        recv, msg = pl.pallas_call(
            functools.partial(kernel, sp, tp, seqs, sub, hd, kvh, group, pairs),
            out_shape=(
                pltpu.VMEM((sp, sub, block), jnp.bfloat16),
                pltpu.VMEM((tp, sp, pairs * ROWS, 2 * hd), jnp.float32),
            ),
            in_specs=[any_spec] * 5,
            out_specs=(vmem_spec, vmem_spec),
            scratch_shapes=[
                pltpu.VMEM(x.shape, jnp.bfloat16),
                pltpu.VMEM(key_weight.shape, jnp.bfloat16),
                pltpu.VMEM(value_weight.shape, jnp.bfloat16),
                pltpu.VMEM((group, pairs, hd), jnp.bfloat16),
                pltpu.VMEM(head_bias.shape, jnp.float32),
                pltpu.VMEM((sp, sub, block), jnp.bfloat16),
                dma((2,)),
                dma((2, KC)),
                dma((2,)),
                dma((sp,)),
                dma((sp,)),
                dma((tp, sp)),
                dma((tp, sp)),
            ],
            compiler_params=pltpu.CompilerParams(
                collective_id=0, has_side_effects=True, vmem_limit_bytes=limit
            ),
        )(x, key_weight, value_weight, queries.transpose(1, 0, 2), head_bias)
        return pl.pallas_call(
            functools.partial(finish, sp, tp, hd, group, pairs),
            out_shape=(
                jax.ShapeDtypeStruct((pairs, sp, sub, 2 * hd), jnp.bfloat16),
                jax.ShapeDtypeStruct((pairs, group * hd), jnp.bfloat16),
            ),
            in_specs=[vmem_spec, vmem_spec],
            out_specs=(any_spec, vmem_spec),
            scratch_shapes=[
                pltpu.VMEM((pairs * ROWS, 2 * hd), jnp.float32),
                dma((sp, pairs)),
            ],
            compiler_params=pltpu.CompilerParams(vmem_limit_bytes=VMEM_BYTES // 4),
        )(recv, msg)

    in_specs = (P(None, ("sp", "tp"), None), P(), P(), P("sp", None, None), P())
    out_specs = (P("sp", None, "tp", None), P("sp", None))
    return jax.shard_map(per_device, mesh=mesh, in_specs=in_specs, out_specs=out_specs, check_vma=False)
```

```python
import functools
import math

import jax
import jax.numpy as jnp
from jax import lax
from jax.experimental import pallas as pl
from jax.experimental.pallas import tpu as pltpu
from jax.sharding import PartitionSpec as P

EPS_NORM = 0.0001
MESH = pl.DeviceIdType.MESH
KC = 4
VMEM_BYTES = 60 * 1024 * 1024
ROWS = 8


def flip(index, k):
    bit = 1
    while bit <= k:
        if k & bit:
            index = index + (1 - 2 * ((index // bit) % 2)) * bit
        bit *= 2
    return index


def packed_rows(pairs, group):
    return pairs * group // 8 * 8 + 8


def kernel(
    sp, tp, seqs, sub, hd, kvh, group, pairs,
    x_hbm, wk_hbm, wv_hbm, q_hbm, bias_hbm,
    recv, msg,
    x_v, wk_v, wv_v, q_v, bias_v, send,
    x_sem, w_sem, small_sem, send_sem, recv_sem, msend_sem, mrecv_sem,
):
    me = lax.axis_index("sp")
    mt = lax.axis_index("tp")
    per_seq = kvh // pairs
    width = x_hbm.shape[1]
    kc = width // KC
    half_rows = seqs * sub // 2

    barrier = pltpu.get_barrier_semaphore()
    for k in range(1, sp):
        pl.semaphore_signal(barrier, inc=1, device_id={"sp": flip(me, k)}, device_id_type=MESH)
    for k in range(1, tp):
        pl.semaphore_signal(barrier, inc=1, device_id={"tp": lax.rem(mt + k, tp)}, device_id_type=MESH)

    top = me // (sp // 2)
    far_row = pl.multiple_of((1 - top) * half_rows, half_rows)
    near_row = pl.multiple_of(top * half_rows, half_rows)

    x_far = pltpu.make_async_copy(x_hbm.at[pl.ds(far_row, half_rows)], x_v.at[pl.ds(far_row, half_rows)], x_sem.at[0])
    x_near = pltpu.make_async_copy(x_hbm.at[pl.ds(near_row, half_rows)], x_v.at[pl.ds(near_row, half_rows)], x_sem.at[1])
    x_far.start()
    w_copies = []
    for c in range(KC):
        rows = pl.ds(c * kc, kc)
        a = pltpu.make_async_copy(wk_hbm.at[rows], wk_v.at[rows], w_sem.at[0, c])
        b = pltpu.make_async_copy(wv_hbm.at[rows], wv_v.at[rows], w_sem.at[1, c])
        a.start()
        b.start()
        w_copies.append((a, b))
    x_near.start()
    q_copy = pltpu.make_async_copy(q_hbm, q_v, small_sem.at[0])
    bias_copy = pltpu.make_async_copy(bias_hbm, bias_v, small_sem.at[1])
    q_copy.start()
    bias_copy.start()

    def pieces(keys, values, i, part):
        out = []
        for p in range(pairs):
            c0 = (part * pairs + p) * hd
            out.append(keys[i * sub:(i + 1) * sub, c0:c0 + hd])
            out.append(values[i * sub:(i + 1) * sub, c0:c0 + hd])
        return jnp.concatenate(out, axis=1).astype(jnp.bfloat16)

    x_far.wait()
    keys = values = None
    for c in range(KC):
        w_copies[c][0].wait()
        w_copies[c][1].wait()
        xc = x_v[pl.ds(far_row, half_rows), c * kc:(c + 1) * kc]
        dk = jnp.dot(xc, wk_v[c * kc:(c + 1) * kc, :], preferred_element_type=jnp.float32)
        dv = jnp.dot(xc, wv_v[c * kc:(c + 1) * kc, :], preferred_element_type=jnp.float32)
        keys = dk if keys is None else keys + dk
        values = dv if values is None else values + dv
    far_base = (1 - top) * (sp // 2)
    for i in range(seqs // 2):
        for part in range(per_seq):
            send[pl.ds(far_base + i * per_seq + part, 1)] = pieces(keys, values, i, part)[None]

    pl.semaphore_wait(barrier, sp + tp - 2)

    def block_copy(k):
        to = flip(me, k)
        return pltpu.make_async_remote_copy(
            src_ref=send.at[to], dst_ref=recv.at[me],
            send_sem=send_sem.at[to], recv_sem=recv_sem.at[me],
            device_id={"sp": to}, device_id_type=MESH,
        )

    def arrived(k):
        frm = flip(me, k)
        return pltpu.make_async_remote_copy(
            src_ref=send.at[frm], dst_ref=recv.at[frm],
            send_sem=send_sem.at[frm], recv_sem=recv_sem.at[frm],
            device_id={"sp": frm}, device_id_type=MESH,
        )

    for k in range(sp // 2, sp):
        block_copy(k).start()

    x_near.wait()
    xn = x_v[pl.ds(near_row, half_rows), :]
    keys = jnp.dot(xn, wk_v[...], preferred_element_type=jnp.float32)
    values = jnp.dot(xn, wv_v[...], preferred_element_type=jnp.float32)
    near_base = top * (sp // 2)
    for i in range(seqs // 2):
        for part in range(per_seq):
            send[pl.ds(near_base + i * per_seq + part, 1)] = pieces(keys, values, i, part)[None]
    for k in range(1, sp // 2):
        block_copy(k).start()
    recv[pl.ds(me, 1)] = send[pl.ds(me, 1)]

    q_copy.wait()
    bias_copy.wait()
    h0 = lax.rem(me * pairs, kvh)
    eye = lax.broadcasted_iota(jnp.int32, (ROWS, group), 0) == lax.broadcasted_iota(jnp.int32, (ROWS, group), 1)
    q_pads = []
    shifts = []
    for p in range(pairs):
        qp = q_v[:, p, :].astype(jnp.float32)
        qp = jnp.concatenate([qp, jnp.zeros((group, hd), jnp.float32)], axis=1)
        qp = jnp.concatenate([qp, jnp.zeros((ROWS - group, 2 * hd), jnp.float32)], axis=0)
        q_pads.append(qp.astype(jnp.bfloat16))
        row = bias_v[pl.ds(h0 + p, 1), :]
        shifts.append(jnp.sum(jnp.where(eye, jnp.broadcast_to(row, (ROWS, group)), 0.0), axis=1, keepdims=True))
    shift = jnp.concatenate(shifts, axis=0)
    scale = 1.0 / math.sqrt(hd)
    later = lax.broadcasted_iota(jnp.int32, (sub, 256), 0)
    column = lax.broadcasted_iota(jnp.int32, (sub, 256), 1)
    tri = ((later > column) | (column >= 128)).astype(jnp.float32).astype(jnp.bfloat16)
    left_half = lax.broadcasted_iota(jnp.int32, (pairs * ROWS, 2 * hd), 1) < hd

    def msg_copy(b, t):
        return pltpu.make_async_remote_copy(
            src_ref=msg.at[mt, b], dst_ref=msg.at[mt, b],
            send_sem=msend_sem.at[t, b], recv_sem=mrecv_sem.at[mt, b],
            device_id={"tp": t}, device_id_type=MESH,
        )

    def msg_arrived(b, t):
        return pltpu.make_async_remote_copy(
            src_ref=msg.at[t, b], dst_ref=msg.at[t, b],
            send_sem=msend_sem.at[t, b], recv_sem=mrecv_sem.at[t, b],
            device_id={"tp": t}, device_id_type=MESH,
        )

    def attend(b):
        scores = []
        for p in range(pairs):
            kv = recv[b, :, p * 2 * hd:(p + 1) * 2 * hd]
            scores.append(lax.dot_general(q_pads[p], kv, (((1,), (1,)), ((), ())), preferred_element_type=jnp.float32))
        s = jnp.concatenate(scores, axis=0) * scale + shift
        low = jnp.log1p(jnp.exp(-jnp.abs(s)))
        keep = -(jnp.maximum(s, 0.0) + low)
        sig = jnp.minimum(s, 0.0) - low
        hi = keep.astype(jnp.bfloat16)
        rest = keep - hi.astype(jnp.float32)
        mid = rest.astype(jnp.bfloat16)
        lo = (rest - mid.astype(jnp.float32)).astype(jnp.bfloat16)
        n = pairs * ROWS
        sums = (
            jnp.dot(hi, tri, preferred_element_type=jnp.float32)
            + jnp.dot(mid, tri, preferred_element_type=jnp.float32)
            + jnp.dot(lo, tri, preferred_element_type=jnp.float32)
        )
        weights = jnp.exp(sig + sums[:, :sub]).astype(jnp.bfloat16)
        reads = []
        for p in range(pairs):
            kv = recv[b, :, p * 2 * hd:(p + 1) * 2 * hd]
            reads.append(jnp.dot(weights[p * ROWS:(p + 1) * ROWS], kv, preferred_element_type=jnp.float32))
        read = jnp.concatenate(reads, axis=0)
        both = jnp.where(left_half, sums[:, 128:128 + 2 * hd], read)
        packed = [both[p * ROWS:p * ROWS + group] for p in range(pairs)]
        packed.append(jnp.zeros((packed_rows(pairs, group) - pairs * group, 2 * hd), jnp.float32))
        msg[mt, b] = jnp.concatenate(packed, axis=0)
        for t in range(1, tp):
            msg_copy(b, lax.rem(mt + t, tp)).start()

    order = [0] + list(range(1, sp))
    for k in order:
        b = flip(me, k)
        if k:
            arrived(k).wait_recv()
        attend(b)

    for b in range(sp):
        for t in range(1, tp):
            msg_arrived(b, lax.rem(mt + t, tp)).wait_recv()

    for k in range(1, sp):
        block_copy(k).wait_send()
    for b in range(sp):
        for t in range(1, tp):
            msg_copy(b, lax.rem(mt + t, tp)).wait_send()


def finish(sp, tp, hd, group, pairs, recv, msg, stored_hbm, first_hbm, fin, first_v, out_sem, first_sem):
    copies = [
        pltpu.make_async_copy(recv.at[b, :, pl.ds(p * 2 * hd, 2 * hd)], stored_hbm.at[p, b], out_sem.at[b, p])
        for b in range(sp)
        for p in range(pairs)
    ]
    for copy in copies:
        copy.start()
    left_half = lax.broadcasted_iota(jnp.int32, (packed_rows(pairs, group), 2 * hd), 1) < hd

    def add_block(i, carry):
        total, acc = carry
        b = sp - 1 - i
        for j in range(tp - 1, -1, -1):
            m = msg[j, b]
            total = total + jnp.exp(acc) * m
            acc = acc + pltpu.roll(m, hd, 1)
        return total, acc

    zero = jnp.zeros((packed_rows(pairs, group), 2 * hd), jnp.float32)
    total, _ = lax.fori_loop(0, sp, add_block, (zero, zero), unroll=True)
    total = jnp.where(left_half, 0.0, total)
    squares = jnp.sum(total * total, axis=1, keepdims=True) * (1.0 / hd)
    fin[...] = pltpu.roll(total * lax.rsqrt(squares + EPS_NORM), hd, 1)
    cols = [fin[pl.ds(g, pairs, stride=group), :][:, :hd] for g in range(group)]
    first_v[...] = jnp.concatenate(cols, axis=1).astype(first_v.dtype)
    first_copy = pltpu.make_async_copy(first_v, first_hbm, first_sem)
    first_copy.start()

    for copy in copies:
        copy.wait()
    first_copy.wait()


def solution(mesh):
    sp, tp = mesh.shape["sp"], mesh.shape["tp"]

    def per_device(layer_input, key_weight, value_weight, queries, head_bias):
        seqs, sub, width = layer_input.shape
        pairs, group, hd = queries.shape
        kvh = head_bias.shape[0]
        x = layer_input.reshape(seqs * sub, width)
        block = pairs * 2 * hd
        any_spec = pl.BlockSpec(memory_space=pltpu.HBM)
        dma = pltpu.SemaphoreType.DMA
        handed = sp * sub * block * 2 + tp * sp * packed_rows(pairs, group) * 2 * hd * 4
        limit = VMEM_BYTES - handed
        vmem_spec = pl.BlockSpec(memory_space=pltpu.VMEM)
        recv, msg = pl.pallas_call(
            functools.partial(kernel, sp, tp, seqs, sub, hd, kvh, group, pairs),
            out_shape=(
                pltpu.VMEM((sp, sub, block), jnp.bfloat16),
                pltpu.VMEM((tp, sp, packed_rows(pairs, group), 2 * hd), jnp.float32),
            ),
            in_specs=[any_spec] * 5,
            out_specs=(vmem_spec, vmem_spec),
            scratch_shapes=[
                pltpu.VMEM(x.shape, jnp.bfloat16),
                pltpu.VMEM(key_weight.shape, jnp.bfloat16),
                pltpu.VMEM(value_weight.shape, jnp.bfloat16),
                pltpu.VMEM((group, pairs, hd), jnp.bfloat16),
                pltpu.VMEM(head_bias.shape, jnp.float32),
                pltpu.VMEM((sp, sub, block), jnp.bfloat16),
                dma((2,)),
                dma((2, KC)),
                dma((2,)),
                dma((sp,)),
                dma((sp,)),
                dma((tp, sp)),
                dma((tp, sp)),
            ],
            compiler_params=pltpu.CompilerParams(
                collective_id=0, has_side_effects=True, vmem_limit_bytes=limit
            ),
        )(x, key_weight, value_weight, queries.transpose(1, 0, 2), head_bias)
        return pl.pallas_call(
            functools.partial(finish, sp, tp, hd, group, pairs),
            out_shape=(
                jax.ShapeDtypeStruct((pairs, sp, sub, 2 * hd), jnp.bfloat16),
                jax.ShapeDtypeStruct((pairs, group * hd), jnp.bfloat16),
            ),
            in_specs=[vmem_spec, vmem_spec],
            out_specs=(any_spec, any_spec),
            scratch_shapes=[
                pltpu.VMEM((packed_rows(pairs, group), 2 * hd), jnp.float32),
                pltpu.VMEM((pairs, group * hd), jnp.bfloat16),
                dma((sp, pairs)),
                dma(()),
            ],
            compiler_params=pltpu.CompilerParams(vmem_limit_bytes=VMEM_BYTES // 4),
        )(recv, msg)

    in_specs = (P(None, ("sp", "tp"), None), P(), P(), P("sp", None, None), P())
    out_specs = (P("sp", None, "tp", None), P("sp", None))
    return jax.shard_map(per_device, mesh=mesh, in_specs=in_specs, out_specs=out_specs, check_vma=False)
```
